32 devices in a mesh: fs: 2 (over core), tp: 16 (over z, y, x).
Axes of the slice: x: 2, y: 2, z: 4, core: 2. Of those that a mesh axis runs over, the one named last changes fastest.
Arguments:
- trained_gate: float32 [16, 504, 2048], P(None, 'fs', 'tp'), may hold values from -0.125 to 0.125
- trained_up: float32 [16, 504, 2048], P(None, 'fs', 'tp'), may hold values from -0.125 to 0.125
- trained_down: float32 [16, 504, 2048], P(None, 'fs', 'tp'), may hold values from -0.25 to 0.25
- trained_shared_gate: float32 [504, 2048], P('fs', 'tp'), may hold values from -0.125 to 0.125
- trained_shared_up: float32 [504, 2048], P('fs', 'tp'), may hold values from -0.125 to 0.125
- trained_shared_down: float32 [504, 2048], P('fs', 'tp'), may hold values from -0.25 to 0.25
- ffn_gain: float32 [2048], P('tp'), may hold values from 0.1 to 1.9
- prompt_tokens: bfloat16 [512, 2048], P('fs'), may hold values from -6 to 6
- expert_ids: int32 [512, 8], P('fs'), may hold values from 0 to 15, all different within a row; in each aligned block of 256 rows (0 to 255, 256 to 511, ...) at most 256 rows name the same one
- route_scores: float32 [512, 8], P('fs'), may hold values from 0.05 to 1
Outputs:
- served_gate: bfloat16 [16, 504, 2048], P('tp')
- served_up: bfloat16 [16, 504, 2048], P('tp')
- served_down: bfloat16 [16, 504, 2048], P('tp')
- served_shared_gate: bfloat16 [504, 2048], P(None, 'tp')
- served_shared_up: bfloat16 [504, 2048], P(None, 'tp')
- served_shared_down: bfloat16 [504, 2048], P(None, 'tp')
- mixture_out: bfloat16 [512, 2048], P('fs', 'tp')
The draws below stay inside these ranges and needn't reach their ends.
Inputs may be any that keep to these rules, and one draw needn't show every extreme that they name: `expert_ids`: each row names 8 different experts, and every expert is named by some row. Within the 256 rows of one index of fs no expert is named by more than 256 rows, and in every draw some expert is named by exactly 256 rows of some index of fs.
All inputs are finite; a program needn't handle non-finite values.
Results may differ from the reference program's by a relative error of at most 0.0082.
Values may be sent and summed in bfloat16 or wider, within the bound.
A program may use at most 64 MiB of HBM per device.

```python
import math
import jax
import jax.numpy as jnp
import numpy as np
from jax import lax

D = 2048
FF = 504
TOP_K = 8
TOK = 256
EXPERTS = 16
CAP = 256
TOKENS = 512
N_FS = 2


def level_of(key, shape, split, low, largest):
    gain = 1.0
    for axis_at, parts in split:
        heights = jax.random.uniform(jax.random.fold_in(jax.random.fold_in(key, 6), axis_at), (parts,), jnp.float32, low / len(split), largest / len(split))
        gain = gain * jnp.repeat(jnp.exp(heights), shape[axis_at] // parts).reshape((-1,) + (1,) * (len(shape) - 1 - axis_at))
    return gain


def assign_block(key, own, number, rows, count, top, reach, lean):
    order = jax.random.permutation(key, count)
    crowded, common = shares(count, rows * top, reach, lean, True), shares(count, rows * top, reach, lean, False)
    places = jnp.arange(count)

    def named(lengths, rotation):
        used = int((lengths > 0).sum())
        fixed = max(1, used // 4)
        moved = fixed + (places - fixed + rotation * (used - fixed)) % max(1, count - fixed)
        return jnp.zeros((count,), jnp.int32).at[order[jnp.where(places < fixed, places, moved)]].set(jnp.asarray(lengths, jnp.int32))

    lengths = jnp.where(number % 4 == 0, named(crowded, number // 4), named(common, number - number // 4 - 1))
    mixed = jax.random.permutation(jax.random.fold_in(own, 3), count)
    donor, sink = mixed[0:count // 2 * 2:2], mixed[1:count // 2 * 2:2]
    slack = jnp.minimum(lengths[donor] - 1, reach - lengths[sink]) // 2
    slack = jnp.where((donor == order[0]) | (sink == order[0]) | (lengths[sink] == 0), 0, jnp.maximum(slack, 0))
    moved = jax.random.randint(jax.random.fold_in(own, 4), (count // 2,), 0, 1 << 20) % (slack + 1)
    lengths = lengths.at[donor].add(-moved).at[sink].add(moved)
    labels = jnp.searchsorted(jnp.cumsum(lengths), jnp.arange(rows * top), side="right").astype(jnp.int32)
    table = labels.reshape(top, rows).T
    table = table[jax.random.permutation(jax.random.fold_in(own, 1), rows)]
    rotation = jax.random.randint(jax.random.fold_in(own, 2), (rows, 1), 0, top)
    return jnp.take_along_axis(table, (jnp.arange(top)[None, :] + rotation) % top, axis=1)


def shares(count, total, most, lean, full):
    portions = [(1 << 20) // math.isqrt(rank ** lean) + 1 for rank in range(1, count + 1)]
    largest = most if full else min(most, max(-(-total // count), total * portions[0] // sum(portions)))
    least = 1 if total - largest >= count - 1 else 0
    counts, rest = [largest] + [least] * (count - 1), total - largest - least * (count - 1)
    while rest > 0:
        movable = [i for i in range(1, count) if counts[i] < largest] or [i for i in range(1, count) if counts[i] < most]
        mass, budget = sum([portions[i] for i in movable]), rest
        for i in movable:
            addition = min(most - counts[i], max(1, budget * portions[i] // mass), rest)
            counts[i] = counts[i] + addition
            rest = rest - addition
    return np.array(counts)


def scatter_about(key, shape, width, most, cuts=(), held_as=jnp.bfloat16):
    entries = width * jax.random.normal(key, shape, jnp.float32)
    if cuts:
        entries = entries * level_of(key, shape, cuts, -0.22, 0.18)
    return jnp.clip(entries, -most, most).astype(held_as)


def setup_inputs(seed: int = 0) -> dict:
    seeds = jax.random.split(jax.random.key(seed), 11)
    trained_gate = scatter_about(seeds[0], (EXPERTS, FF, D), D ** -0.5, 0.125, ((1, 2), (2, 16)), jnp.float32)
    trained_up = scatter_about(seeds[1], (EXPERTS, FF, D), D ** -0.5, 0.125, ((1, 2), (2, 16)), jnp.float32)
    trained_down = scatter_about(seeds[2], (EXPERTS, FF, D), FF ** -0.5, 0.25, ((1, 2), (2, 16)), jnp.float32)
    trained_shared_gate = scatter_about(seeds[3], (FF, D), D ** -0.5, 0.125, ((0, 2), (1, 16)), jnp.float32)
    trained_shared_up = scatter_about(seeds[4], (FF, D), D ** -0.5, 0.125, ((0, 2), (1, 16)), jnp.float32)
    trained_shared_down = scatter_about(seeds[5], (FF, D), FF ** -0.5, 0.25, ((0, 2), (1, 16)), jnp.float32)
    ffn_gain = jnp.clip(1.0 + 0.18 * jax.random.normal(seeds[6], (D,), jnp.float32), 0.1, 1.9)
    prompt_tokens = scatter_about(seeds[7], (TOKENS, D), 1.0, 6.0, ((0, 2),))
    expert_ids_keys = jax.random.split(jax.random.fold_in(seeds[8], 1), TOKENS // TOK)
    expert_ids_turns = jax.random.permutation(jax.random.fold_in(seeds[8], 3), TOKENS // TOK)
    expert_ids = jax.vmap(lambda own, number: assign_block(jax.random.fold_in(seeds[8], 2), own, number, TOK, EXPERTS, TOP_K, CAP, 1))(expert_ids_keys, expert_ids_turns).reshape((TOKENS, TOP_K))
    route_scores = jnp.clip(jnp.exp(math.log(1.0) - 2.9957323 * jax.random.uniform(seeds[9], (TOKENS, TOP_K), jnp.float32) ** level_of(seeds[9], (TOKENS, TOP_K), ((0, 2),), -0.2, 0.2)), 0.05, 1.0)
    return {"trained_gate": trained_gate, "trained_up": trained_up, "trained_down": trained_down, "trained_shared_gate": trained_shared_gate, "trained_shared_up": trained_shared_up, "trained_shared_down": trained_shared_down, "ffn_gain": ffn_gain, "prompt_tokens": prompt_tokens, "expert_ids": expert_ids, "route_scores": route_scores}


EPSILON = 1e-06
ROUTED_SCALE = 2.5

def contract(left, right):
    return lax.dot_general(left, right, (((1,), (1,)), ((), ())), preferred_element_type=jnp.float32)

def reference(trained_gate, trained_up, trained_down, trained_shared_gate, trained_shared_up, trained_shared_down, ffn_gain, prompt_tokens, expert_ids, route_scores):
    served_gate = (trained_gate * ffn_gain[None, None, :]).astype(jnp.bfloat16)
    served_up = (trained_up * ffn_gain[None, None, :]).astype(jnp.bfloat16)
    served_down = trained_down.astype(jnp.bfloat16)
    served_shared_gate = (trained_shared_gate * ffn_gain[None, :]).astype(jnp.bfloat16)
    served_shared_up = (trained_shared_up * ffn_gain[None, :]).astype(jnp.bfloat16)
    served_shared_down = trained_shared_down.astype(jnp.bfloat16)
    tokens_float = prompt_tokens.astype(jnp.float32)
    normed = (tokens_float * lax.rsqrt(lax.optimization_barrier(jnp.mean(tokens_float * tokens_float, axis=1, keepdims=True)) + EPSILON)).astype(jnp.bfloat16)
    route_weight = ROUTED_SCALE * route_scores / lax.optimization_barrier(jnp.sum(route_scores, axis=1, keepdims=True))
    token_total = prompt_tokens.shape[0]
    slot_total = N_FS * CAP
    token_range = jnp.arange(token_total, dtype=jnp.int32)

    def one_expert(routed, inputs):
        expert_index, gate_weight, up_weight, down_weight = inputs
        chosen = expert_ids == expert_index
        token_weight = lax.optimization_barrier(jnp.sum(jnp.where(chosen, route_weight, 0.0), axis=1))
        present = jnp.any(chosen, axis=1)
        position = (jnp.cumsum(present.astype(jnp.int32)) - 1).astype(jnp.int32)
        target = jnp.where(present, position, slot_total).astype(jnp.int32)
        slot_token = jnp.zeros((slot_total + 1,), jnp.int32).at[target].set(token_range)[:slot_total]
        slot_rows = jnp.take(normed, slot_token, axis=0)
        gate_pre = contract(slot_rows, gate_weight)
        up_pre = contract(slot_rows, up_weight)
        expert_act = (jax.nn.silu(gate_pre) * up_pre).astype(jnp.bfloat16)
        expert_out = jnp.dot(expert_act, down_weight, preferred_element_type=jnp.float32)
        picked = jnp.take(expert_out, jnp.maximum(position, 0), axis=0)
        return (routed + jnp.where(present[:, None], picked * token_weight[:, None], 0.0), None)
    expert_range = jnp.arange(EXPERTS, dtype=jnp.int32)
    routed, _ = lax.scan(one_expert, jnp.zeros((token_total, D), jnp.float32), (expert_range, served_gate, served_up, served_down))
    shared_gate_pre = contract(normed, served_shared_gate)
    shared_up_pre = contract(normed, served_shared_up)
    shared_act = (jax.nn.silu(shared_gate_pre) * shared_up_pre).astype(jnp.bfloat16)
    shared_out = jnp.dot(shared_act, served_shared_down, preferred_element_type=jnp.float32)
    mixture_out = (routed + shared_out).astype(jnp.bfloat16)
    return (served_gate, served_up, served_down, served_shared_gate, served_shared_up, served_shared_down, mixture_out)
```

```python
import functools

import jax
import jax.numpy as jnp
from jax import lax
from jax.experimental import pallas as pl
from jax.experimental.pallas import tpu as pltpu
from jax.sharding import PartitionSpec as P

EPSILON = 1e-06
ROUTED_SCALE = 2.5


def contract(left, right):
    return lax.dot_general(
        left, right, (((1,), (1,)), ((), ())), preferred_element_type=jnp.float32
    )


def plain_on_device(
    trained_gate,
    trained_up,
    trained_down,
    trained_shared_gate,
    trained_shared_up,
    trained_shared_down,
    ffn_gain,
    prompt_tokens,
    expert_ids,
    route_scores,
):
    gate_cast = (trained_gate * ffn_gain[None, None, :]).astype(jnp.bfloat16)
    up_cast = (trained_up * ffn_gain[None, None, :]).astype(jnp.bfloat16)
    down_cast = trained_down.astype(jnp.bfloat16)
    shared_gate_cast = (trained_shared_gate * ffn_gain[None, :]).astype(jnp.bfloat16)[None]
    shared_up_cast = (trained_shared_up * ffn_gain[None, :]).astype(jnp.bfloat16)[None]
    shared_down_cast = trained_shared_down.astype(jnp.bfloat16)[None]
    expert_gate, expert_up, expert_down = (
        lax.all_to_all(gate_cast, "tp", split_axis=0, concat_axis=2, tiled=True),
        lax.all_to_all(up_cast, "tp", split_axis=0, concat_axis=2, tiled=True),
        lax.all_to_all(down_cast, "tp", split_axis=0, concat_axis=2, tiled=True),
    )
    token_count, model_width = prompt_tokens.shape
    tokens_float = prompt_tokens.astype(jnp.float32)
    normed = (
        tokens_float
        * lax.rsqrt(jnp.mean(tokens_float * tokens_float, axis=1, keepdims=True) + EPSILON)
    ).astype(jnp.bfloat16)
    column_width = ffn_gain.shape[0]
    expert_index = lax.axis_index("tp")
    normed_cols = lax.dynamic_slice_in_dim(normed, expert_index * column_width, column_width, 1)
    expert_count = lax.axis_size("tp")
    top_count = expert_ids.shape[1]
    capacity = min(token_count, 5 * token_count * top_count // (2 * expert_count))
    route_weight = ROUTED_SCALE * route_scores / jnp.sum(route_scores, axis=1, keepdims=True)
    chosen = expert_ids == expert_index
    present = jnp.any(chosen, axis=1)
    position = jnp.cumsum(present.astype(jnp.int32)) - 1
    slot_match = (position[None, :] == jnp.arange(capacity, dtype=jnp.int32)[:, None]) & present[
        None, :
    ]
    slot_token = jnp.sum(
        jnp.where(slot_match, jnp.arange(token_count, dtype=jnp.int32)[None, :], 0), axis=1
    )
    slot_rows = jnp.take(normed, slot_token, axis=0)
    gathered = (
        lax.all_gather(expert_gate, "fs", axis=1, tiled=True),
        lax.all_gather(expert_up, "fs", axis=1, tiled=True),
        lax.all_gather(expert_down, "fs", axis=1, tiled=True),
        lax.all_gather(shared_gate_cast, "fs", axis=1, tiled=True),
        lax.all_gather(shared_up_cast, "fs", axis=1, tiled=True),
        lax.all_gather(shared_down_cast, "fs", axis=1, tiled=True),
    )
    gate_full, up_full, down_full, sgate_full, sup_full, sdown_full = gathered
    gate_pre = contract(slot_rows, gate_full[0])
    up_pre = contract(slot_rows, up_full[0])
    sgate_part = contract(normed_cols, sgate_full[0])
    sup_part = contract(normed_cols, sup_full[0])
    expert_act = (jax.nn.silu(gate_pre) * up_pre).astype(jnp.bfloat16)
    shared_gate_pre, shared_up_pre = lax.psum((sgate_part, sup_part), "tp")
    shared_act = (jax.nn.silu(shared_gate_pre) * shared_up_pre).astype(jnp.bfloat16)
    expert_out = jnp.dot(expert_act, down_full[0], preferred_element_type=jnp.float32)
    shared_out = jnp.dot(shared_act, sdown_full[0], preferred_element_type=jnp.float32)
    arrived = lax.all_to_all(expert_out, "tp", split_axis=1, concat_axis=0, tiled=True)
    arrived = arrived.reshape(expert_count, capacity, column_width)

    def add_expert(total, inputs):
        source_index, source_rows = inputs
        source_chosen = expert_ids == source_index
        source_weight = jnp.sum(jnp.where(source_chosen, route_weight, 0.0), axis=1)
        source_present = jnp.any(source_chosen, axis=1)
        source_position = jnp.cumsum(source_present.astype(jnp.int32)) - 1
        source_picked = jnp.take(source_rows, jnp.maximum(source_position, 0), axis=0)
        return (
            total + jnp.where(source_present[:, None], source_picked * source_weight[:, None], 0.0),
            None,
        )

    routed_cols, _ = lax.scan(
        add_expert,
        jnp.zeros((token_count, column_width), jnp.float32),
        (jnp.arange(expert_count, dtype=jnp.int32), arrived),
    )
    mixture = (routed_cols + shared_out).astype(jnp.bfloat16)
    return (gate_full, up_full, down_full, sgate_full[0], sup_full[0], sdown_full[0], mixture)

TILE = 16
VMEM_BYTES = 67000000


def geometry(n, n_fs, experts, rows, columns):
    block = -(-rows // TILE) * TILE
    edge = block - rows
    if n_fs != 2 or experts != n or columns % 128 or n % 4 or not 0 < edge < 8 or block % (TILE * n):
        return None
    if n // 4 != 4:
        return None
    return block, edge, block // n


def kernel(
    n,
    block,
    edge,
    piece,
    gate_in,
    up_in,
    down_in,
    sgate_in,
    sup_in,
    sdown_in,
    gain_in,
    tokens_in,
    ids_in,
    scores_in,
    gate_out,
    up_out,
    down_out,
    sgate_out,
    sup_out,
    sdown_out,
    mix_out,
    gain_ref,
    tokens_ref,
    ids_ref,
    scores_ref,
    raw,
    shared_raw,
    rim,
    shared_rim,
    packed,
    shared_half,
    held,
    normed,
    gate_acc,
    up_acc,
    act,
    parts,
    plane,
    line,
    total,
    mix,
    mix_sem,
    small_sem,
    load_sem,
    shared_load_sem,
    rim_send,
    rim_recv,
    shared_rim_send,
    shared_rim_recv,
    shared_send,
    shared_recv,
    shared_keep,
    send_sem,
    recv_sem,
    pass_send,
    pass_recv,
    keep_sem,
    plane_send,
    plane_recv,
    line_send,
    line_recv,
):
    routed_in = (gate_in, up_in, down_in)
    shared_in = (sgate_in, sup_in, sdown_in)
    routed_out = (gate_out, up_out, down_out)
    shared_out = (sgate_out, sup_out, sdown_out)
    me = lax.axis_index("tp")
    core = lax.axis_index("fs")
    other = 1 - core
    inner = 4
    outer = n // inner
    my_a, my_b = me // inner, me % inner
    rows, columns = sgate_in.shape
    chunks = 4 if rows % 4 == 0 else 1
    chunk = rows // chunks * n
    first = core == 0

    def load(m, at):
        here = pl.ds(at * chunk, chunk)
        return pltpu.make_async_copy(routed_in[m].at[here], raw.at[m, here], load_sem.at[m, at])

    def load_shared(m):
        return pltpu.make_async_copy(shared_in[m], shared_raw.at[m], shared_load_sem.at[m])

    def to_peer(m, dst):
        return pltpu.make_async_remote_copy(
            src_ref=packed.at[m, dst],
            dst_ref=held.at[m, me, core],
            send_sem=send_sem.at[m, dst],
            recv_sem=recv_sem.at[m, me],
            device_id={"tp": dst},
            device_id_type=pl.DeviceIdType.MESH,
        )

    def from_peer(m, src):
        return pltpu.make_async_remote_copy(
            src_ref=packed.at[m, src],
            dst_ref=held.at[m, src, core],
            send_sem=send_sem.at[m, src],
            recv_sem=recv_sem.at[m, src],
            device_id={"tp": src},
            device_id_type=pl.DeviceIdType.MESH,
        )

    def own(m):
        return pltpu.make_async_copy(packed.at[m, me], held.at[m, me, core], recv_sem.at[m, me])

    def to_core(m, src, half):
        return pltpu.make_async_remote_copy(
            src_ref=held.at[m, src, half],
            dst_ref=held.at[m, src, half],
            send_sem=pass_send.at[m, src],
            recv_sem=pass_recv.at[m, src],
            device_id={"fs": other},
            device_id_type=pl.DeviceIdType.MESH,
        )

    def keep(m, src, half):
        return pltpu.make_async_copy(
            held.at[m, src, half, pl.ds(0, block)],
            routed_out[m].at[
                pl.ds(half * block, block), pl.ds(pl.multiple_of(src * columns, 128), columns)
            ],
            keep_sem.at[m, src, half],
        )

    def rim_copy(m):
        return pltpu.make_async_remote_copy(
            src_ref=raw.at[m, pl.ds(0, edge * n)],
            dst_ref=rim.at[m],
            send_sem=rim_send.at[m],
            recv_sem=rim_recv.at[m],
            device_id={"fs": other},
            device_id_type=pl.DeviceIdType.MESH,
        )

    def shared_rim_copy(m):
        return pltpu.make_async_remote_copy(
            src_ref=shared_raw.at[m, pl.ds(0, 8)],
            dst_ref=shared_rim.at[m],
            send_sem=shared_rim_send.at[m],
            recv_sem=shared_rim_recv.at[m],
            device_id={"fs": other},
            device_id_type=pl.DeviceIdType.MESH,
        )

    def shared_copy(m, half):
        return pltpu.make_async_remote_copy(
            src_ref=shared_half.at[m, half],
            dst_ref=shared_half.at[m, half],
            send_sem=shared_send.at[m],
            recv_sem=shared_recv.at[m],
            device_id={"fs": other},
            device_id_type=pl.DeviceIdType.MESH,
        )

    def keep_shared(m, half):
        return pltpu.make_async_copy(
            shared_half.at[m, half],
            shared_out[m].at[pl.ds(half * block, block)],
            shared_keep.at[m, half],
        )

    def to_plane(a, b):
        return pltpu.make_async_remote_copy(
            src_ref=parts.at[a, b],
            dst_ref=plane.at[my_b, a],
            send_sem=plane_send.at[a, b],
            recv_sem=plane_recv.at[my_b, a],
            device_id={"tp": my_a * inner + b},
            device_id_type=pl.DeviceIdType.MESH,
        )

    def from_plane(a, b):
        return pltpu.make_async_remote_copy(
            src_ref=parts.at[a, b],
            dst_ref=plane.at[b, a],
            send_sem=plane_send.at[a, b],
            recv_sem=plane_recv.at[b, a],
            device_id={"tp": my_a * inner + b},
            device_id_type=pl.DeviceIdType.MESH,
        )

    def to_line(a):
        return pltpu.make_async_remote_copy(
            src_ref=plane.at[my_b, a],
            dst_ref=line.at[my_a],
            send_sem=line_send.at[a],
            recv_sem=line_recv.at[my_a],
            device_id={"tp": a * inner + my_b},
            device_id_type=pl.DeviceIdType.MESH,
        )

    def from_line(a):
        return pltpu.make_async_remote_copy(
            src_ref=plane.at[my_b, a],
            dst_ref=line.at[a],
            send_sem=line_send.at[a],
            recv_sem=line_recv.at[a],
            device_id={"tp": a * inner + my_b},
            device_id_type=pl.DeviceIdType.MESH,
        )

    def assemble(value, tail):
        cut = block - TILE
        body = jnp.where(first, value[0:cut], value[edge : cut + edge])
        rest = jnp.where(
            first,
            jnp.concatenate([value[cut:rows], tail[0:edge]], axis=0),
            jnp.concatenate(
                [value[cut + edge : rows], jnp.zeros((2 * edge, columns), jnp.float32)], axis=0
            ),
        )
        return cut, body, rest

    smalls = [
        pltpu.make_async_copy(source, target, small_sem.at[at])
        for at, (source, target) in enumerate(
            (
                (gain_in, gain_ref),
                (tokens_in, tokens_ref),
                (ids_in, ids_ref),
                (scores_in, scores_ref),
            )
        )
    ]
    smalls[0].start()
    for m in range(3):
        load_shared(m).start()

    for m in range(3):
        for at in range(chunks):
            load(m, at).start()
    for copy in smalls[1:]:
        copy.start()

    barrier = pltpu.get_barrier_semaphore()
    pl.semaphore_signal(
        barrier, inc=1, device_id={"fs": other}, device_id_type=pl.DeviceIdType.MESH
    )

    def greet(step, carry):
        pl.semaphore_signal(
            barrier,
            inc=1,
            device_id={"tp": (me + step) % n},
            device_id_type=pl.DeviceIdType.MESH,
        )
        return carry

    lax.fori_loop(1, n, greet, 0)
    smalls[0].wait()
    for m in range(3):
        load_shared(m).wait()
    for m in range(2):
        for at in range(chunks):
            load(m, at).wait()
    load(2, 0).wait()
    pl.semaphore_wait(barrier, n)

    @pl.when(core == 1)
    def _():
        for m in range(3):
            shared_rim_copy(m).start()
            rim_copy(m).start()

    @pl.when(core == 0)
    def _():
        for m in range(3):
            shared_rim_copy(m).wait_recv()
            rim_copy(m).wait_recv()

    gain = gain_ref[...]
    for m in range(3):
        scale = gain if m < 2 else jnp.ones_like(gain)
        cut, body, rest = assemble(shared_raw[m], shared_rim[m])
        shared_half[m, core, 0:cut] = (body * scale).astype(jnp.bfloat16)
        shared_half[m, core, cut:block] = (rest * scale).astype(jnp.bfloat16)

    def pack(m, dst):
        scale = gain if m < 2 else jnp.ones_like(gain)
        cut = block - TILE
        start = dst + core * (edge * n)
        body = raw[m, pl.ds(start, cut, stride=n), :]
        end = raw[m, pl.ds(dst + cut * n, rows - cut, stride=n), :]
        head = rim[m, pl.ds(dst, edge, stride=n), :]
        rest = jnp.where(
            first,
            jnp.concatenate([end, head], axis=0),
            jnp.concatenate([end[edge:], jnp.zeros((2 * edge, columns), jnp.float32)], axis=0),
        )
        packed[m, dst, 0:cut] = (body * scale).astype(jnp.bfloat16)
        packed[m, dst, cut:block] = (rest * scale).astype(jnp.bfloat16)
        packed[m, dst, block : block + piece] = shared_half[
            m, core, pl.ds(pl.multiple_of(dst * piece, TILE), piece)
        ]

    mirror = outer - 1 - my_a
    skip = (my_a + outer // 2) % outer
    beside = my_a + 1 - 2 * (my_a % 2)
    edge_plane = ((my_a + 1) // 2 + 1) % 2
    inner_plane = 1 - edge_plane
    third = edge_plane * mirror + inner_plane * skip
    fourth = edge_plane * skip + inner_plane * mirror

    def place_of(step, rising):
        turn = step + rising * (inner - 1 - 2 * step)
        return (2 * turn + 1 - turn // 2) % inner

    def member(plane_at, shift):
        column = (my_b + shift) % 2 + 2 * ((my_b // 2 + shift // 2) % 2)
        return plane_at * inner + column

    def peer_to(plane_at, step):
        return member(plane_at, place_of(step, (plane_at > my_a).astype(jnp.int32)))

    def peer_from(plane_at, step):
        return member(plane_at, place_of(step, (plane_at < my_a).astype(jnp.int32)))

    def send_plane(matrices, plane_at, start):
        def send(step, carry):
            dst = peer_to(plane_at, step)
            for m in matrices:
                pack(m, dst)
                if start:
                    to_peer(m, dst).start()
            return carry

        lax.fori_loop(0, inner, send, 0)

    def send_own(matrices):
        def send(step, carry):
            dst = member(my_a, step)
            for m in matrices:
                pack(m, dst)
                to_peer(m, dst).start()
            return carry

        lax.fori_loop(1, inner, send, 0)

    def launch(m, plane_at):
        def send(step, carry):
            to_peer(m, peer_to(plane_at, step)).start()
            return carry

        lax.fori_loop(0, inner, send, 0)

    for plane_at in (mirror, skip, beside):
        send_plane((0, 1), plane_at, True)
    send_own((0, 1))
    for at in range(1, chunks):
        load(2, at).wait()
    send_plane((2,), beside, True)
    send_own((2,))
    for plane_at in (skip, mirror):
        send_plane((2,), plane_at, False)

    @pl.when(inner_plane == 1)
    def _():
        launch(2, skip)
        launch(2, mirror)

    for m in range(3):
        pack(m, me)
        own(m).start()
        shared_copy(m, core).start()

    for copy in smalls[1:]:
        copy.wait()
    tokens = tokens_ref[...].astype(jnp.float32)
    mean = jnp.mean(tokens * tokens, axis=1, keepdims=True)
    scaled = (tokens * lax.rsqrt(mean + EPSILON)).astype(jnp.bfloat16)
    for i in range(n):
        normed[i] = scaled[:, i * columns : (i + 1) * columns]
    scores = scores_ref[...]
    weights = ROUTED_SCALE * scores / jnp.sum(scores, axis=0, keepdims=True)
    weight = jnp.sum(jnp.where(ids_ref[...] == me, weights, 0.0), axis=0, keepdims=True)
    weight = jnp.transpose(jnp.broadcast_to(weight, (8, weight.shape[1])))[:, 0:1]
    gate_acc[...] = jnp.zeros_like(gate_acc)
    up_acc[...] = jnp.zeros_like(up_acc)

    hidden = 2 * (block + piece)

    def arrive(m, src, local):
        if local:
            own(m).wait()
        else:
            from_peer(m, src).wait_recv()
        to_core(m, src, core).start()
        keep(m, src, core).start()

    def complete(m, src):
        to_core(m, src, other).wait_recv()
        keep(m, src, other).start()
        return held[m, src].reshape(hidden, columns)

    def add(src):
        for m, acc in ((0, gate_acc), (1, up_acc)):
            acc[...] += lax.dot_general(
                normed[src],
                complete(m, src),
                (((1,), (1,)), ((), ())),
                preferred_element_type=jnp.float32,
            )

    def stream(matrices, use, planes, after_group):
        for m in matrices:
            arrive(m, me, True)
        before = me
        for at, plane_at in enumerate((my_a,) + planes):

            def one(step, waiting):
                src = member(my_a, step) if at == 0 else peer_from(plane_at, step)
                for m in matrices:
                    arrive(m, src, False)
                use(waiting)
                return src

            before = lax.fori_loop(1 if at == 0 else 0, inner, one, before)
            after_group(at)
        use(before)

    stream((0, 1), add, (third, beside, fourth), lambda at: None)

    @pl.when(edge_plane == 1)
    def _():
        launch(2, mirror)
        launch(2, skip)

    gate_pre = gate_acc[...]
    place = lax.broadcasted_iota(jnp.int32, gate_pre.shape, 1) % (block + piece)
    share = jnp.where(place < block, weight, 1.0)
    act[...] = (gate_pre / (1.0 + jnp.exp(-gate_pre)) * up_acc[...] * share).astype(jnp.bfloat16)

    def part(src):
        a, b = src // inner, src % inner
        parts[a, b] = jnp.dot(
            act[...], complete(2, src), preferred_element_type=jnp.float32
        ).astype(jnp.bfloat16)

        @pl.when(b != my_b)
        def _():
            to_plane(a, b).start()

    def plane_sum(a):
        result = parts[a, my_b].astype(jnp.float32)
        for db in range(1, inner):
            b = (my_b + db) % inner
            from_plane(a, b).wait_recv()
            result = result + plane[b, a].astype(jnp.float32)
        return result

    def flush(a):
        plane[my_b, a] = plane_sum(a).astype(jnp.bfloat16)
        to_line(a).start()

    down_planes = (beside, third, fourth)

    def after_group(at):
        if at == 1:
            total[...] = plane_sum(my_a)
        if at > 1:
            flush(down_planes[at - 2])

    stream((2,), part, down_planes, after_group)
    flush(fourth)
    for m in range(3):
        shared_copy(m, other).wait_recv()
        for half in range(2):
            keep_shared(m, half).start()
    for da in range(1, outer):
        a = (my_a + da) % outer
        from_line(a).wait_recv()
        total[...] += line[a].astype(jnp.float32)
    mix[...] = total[...].astype(jnp.bfloat16)
    put_mix = pltpu.make_async_copy(mix, mix_out, mix_sem)
    put_mix.start()
    put_mix.wait()

    def drain(src, carry):
        for m in range(3):
            to_core(m, src, core).wait_send()
            keep(m, src, 0).wait()
            keep(m, src, 1).wait()
        return carry

    lax.fori_loop(0, n, drain, 0)

    def drain_sends(step, carry):
        for m in range(3):
            to_peer(m, (me + step) % n).wait_send()
        return carry

    lax.fori_loop(1, n, drain_sends, 0)

    @pl.when(core == 1)
    def _():
        for m in range(3):
            shared_rim_copy(m).wait_send()
            rim_copy(m).wait_send()

    for m in range(3):
        shared_copy(m, core).wait_send()
        for half in range(2):
            keep_shared(m, half).wait()
    for da in range(outer):
        a = (my_a + da) % outer
        for db in range(1, inner):
            to_plane(a, (my_b + db) % inner).wait_send()
        if da:
            to_line(a).wait_send()


def trim(count, pieces, *refs):
    sources, targets, rooms = refs[:count], refs[count : 2 * count], refs[2 * count : 3 * count]
    load_sem, store_sem = refs[3 * count :]
    loads, stores = [], []
    for at in range(count):
        rows = sources[at].shape[0]
        left = targets[at].shape[0]
        size = rows // pieces
        for step in range(pieces):
            here = pl.ds(step * size, size)
            there = pl.ds(step * size, min(size, left - step * size))
            loads.append(
                pltpu.make_async_copy(
                    sources[at].at[here], rooms[at].at[here], load_sem.at[at, step]
                )
            )
            stores.append(
                pltpu.make_async_copy(
                    rooms[at].at[there], targets[at].at[there], store_sem.at[at, step]
                )
            )
    for load in loads:
        load.start()
    for load, store in zip(loads, stores):
        load.wait()
        store.start()
    for store in stores:
        store.wait()


def on_device(n, shape, gate, up, down, sgate, sup, sdown, gain, tokens, ids, scores):
    block, edge, piece = shape
    experts, rows, columns = gate.shape
    count, width = tokens.shape
    hidden = 2 * (block + piece)
    inner, outer = 4, n // 4
    sem = pltpu.SemaphoreType.DMA
    anywhere = pl.BlockSpec(memory_space=pl.ANY)
    hbm = pl.BlockSpec(memory_space=pltpu.HBM)
    vmem = pl.BlockSpec(memory_space=pltpu.VMEM)
    bf16, f32 = jnp.bfloat16, jnp.float32
    full = jax.ShapeDtypeStruct((2 * block, width), bf16)
    thin = jax.ShapeDtypeStruct((2 * block, columns), bf16)
    results = pl.pallas_call(
        functools.partial(kernel, n, block, edge, piece),
        out_shape=(full, full, full, thin, thin, thin, jax.ShapeDtypeStruct((count, columns), bf16)),
        in_specs=[hbm] * 10,
        out_specs=(anywhere,) * 7,
        scratch_shapes=[
            pltpu.VMEM((1, columns), f32),
            pltpu.VMEM(tokens.shape, bf16),
            pltpu.VMEM(ids.shape[::-1], jnp.int32),
            pltpu.VMEM(scores.shape[::-1], f32),
            pltpu.VMEM((3, n * rows, columns), f32),
            pltpu.VMEM((3, rows, columns), f32),
            pltpu.VMEM((3, n * edge, columns), f32),
            pltpu.VMEM((3, 8, columns), f32),
            pltpu.VMEM((3, n, block + piece, columns), bf16),
            pltpu.VMEM((3, 2, block, columns), bf16),
            pltpu.VMEM((3, n, 2, block + piece, columns), bf16),
            pltpu.VMEM((n, count, columns), bf16),
            pltpu.VMEM((count, hidden), f32),
            pltpu.VMEM((count, hidden), f32),
            pltpu.VMEM((count, hidden), bf16),
            pltpu.VMEM((outer, inner, count, columns), bf16),
            pltpu.VMEM((inner, outer, count, columns), bf16),
            pltpu.VMEM((outer, count, columns), bf16),
            pltpu.VMEM((count, columns), f32),
            pltpu.VMEM((count, columns), bf16),
            sem,
            sem((4,)),
            sem((3, n)),
            sem((3,)),
            sem((3,)),
            sem((3,)),
            sem((3,)),
            sem((3,)),
            sem((3,)),
            sem((3,)),
            sem((3, 2)),
            sem((3, n)),
            sem((3, n)),
            sem((3, n)),
            sem((3, n)),
            sem((3, n, 2)),
            sem((outer, inner)),
            sem((inner, outer)),
            sem((outer,)),
            sem((outer,)),
        ],
        compiler_params=pltpu.CompilerParams(
            collective_id=0, has_side_effects=True, vmem_limit_bytes=VMEM_BYTES
        ),
    )(
        *[jnp.transpose(array, (1, 0, 2)).reshape(rows * n, columns) for array in (gate, up, down)],
        sgate,
        sup,
        sdown,
        gain[None, :],
        tokens,
        ids.T,
        scores.T,
    )
    pieces = 2
    whole = pl.pallas_call(
        functools.partial(trim, len(results), pieces),
        out_shape=tuple(
            jax.ShapeDtypeStruct((min(2 * rows, array.shape[0]), array.shape[1]), bf16)
            for array in results
        ),
        in_specs=[anywhere] * len(results),
        out_specs=(hbm,) * len(results),
        scratch_shapes=[pltpu.VMEM(array.shape, bf16) for array in results]
        + [sem((len(results), pieces))] * 2,
        compiler_params=pltpu.CompilerParams(vmem_limit_bytes=VMEM_BYTES),
    )(*results)
    return (*[array[None] for array in whole[:3]], *whole[3:])


def body(n, n_fs, *args):
    experts, rows, columns = args[0].shape
    shape = geometry(n, n_fs, experts, rows, columns)
    if shape is None:
        return plain_on_device(*args)
    return on_device(n, shape, *args)


def solution(mesh):
    placed = (
        P(None, "fs", "tp"),
        P(None, "fs", "tp"),
        P(None, "fs", "tp"),
        P("fs", "tp"),
        P("fs", "tp"),
        P("fs", "tp"),
        P("tp"),
        P("fs", None),
        P("fs", None),
        P("fs", None),
    )
    return jax.shard_map(
        functools.partial(body, mesh.shape["tp"], mesh.shape["fs"]),
        mesh=mesh,
        in_specs=placed,
        out_specs=(
            P("tp", None, None),
            P("tp", None, None),
            P("tp", None, None),
            P(None, "tp"),
            P(None, "tp"),
            P(None, "tp"),
            P("fs", "tp"),
        ),
        check_vma=False,
    )
```

```python
import functools

import jax
import jax.numpy as jnp
from jax import lax
from jax.experimental import pallas as pl
from jax.experimental.pallas import tpu as pltpu
from jax.sharding import PartitionSpec as P

EPSILON = 1e-06
ROUTED_SCALE = 2.5


def contract(left, right):
    return lax.dot_general(
        left, right, (((1,), (1,)), ((), ())), preferred_element_type=jnp.float32
    )


def plain_on_device(
    trained_gate,
    trained_up,
    trained_down,
    trained_shared_gate,
    trained_shared_up,
    trained_shared_down,
    ffn_gain,
    prompt_tokens,
    expert_ids,
    route_scores,
):
    gate_cast = (trained_gate * ffn_gain[None, None, :]).astype(jnp.bfloat16)
    up_cast = (trained_up * ffn_gain[None, None, :]).astype(jnp.bfloat16)
    down_cast = trained_down.astype(jnp.bfloat16)
    shared_gate_cast = (trained_shared_gate * ffn_gain[None, :]).astype(jnp.bfloat16)[None]
    shared_up_cast = (trained_shared_up * ffn_gain[None, :]).astype(jnp.bfloat16)[None]
    shared_down_cast = trained_shared_down.astype(jnp.bfloat16)[None]
    expert_gate, expert_up, expert_down = (
        lax.all_to_all(gate_cast, "tp", split_axis=0, concat_axis=2, tiled=True),
        lax.all_to_all(up_cast, "tp", split_axis=0, concat_axis=2, tiled=True),
        lax.all_to_all(down_cast, "tp", split_axis=0, concat_axis=2, tiled=True),
    )
    token_count, model_width = prompt_tokens.shape
    tokens_float = prompt_tokens.astype(jnp.float32)
    normed = (
        tokens_float
        * lax.rsqrt(jnp.mean(tokens_float * tokens_float, axis=1, keepdims=True) + EPSILON)
    ).astype(jnp.bfloat16)
    column_width = ffn_gain.shape[0]
    expert_index = lax.axis_index("tp")
    normed_cols = lax.dynamic_slice_in_dim(normed, expert_index * column_width, column_width, 1)
    expert_count = lax.axis_size("tp")
    top_count = expert_ids.shape[1]
    capacity = min(token_count, 5 * token_count * top_count // (2 * expert_count))
    route_weight = ROUTED_SCALE * route_scores / jnp.sum(route_scores, axis=1, keepdims=True)
    chosen = expert_ids == expert_index
    present = jnp.any(chosen, axis=1)
    position = jnp.cumsum(present.astype(jnp.int32)) - 1
    slot_match = (position[None, :] == jnp.arange(capacity, dtype=jnp.int32)[:, None]) & present[
        None, :
    ]
    slot_token = jnp.sum(
        jnp.where(slot_match, jnp.arange(token_count, dtype=jnp.int32)[None, :], 0), axis=1
    )
    slot_rows = jnp.take(normed, slot_token, axis=0)
    gathered = (
        lax.all_gather(expert_gate, "fs", axis=1, tiled=True),
        lax.all_gather(expert_up, "fs", axis=1, tiled=True),
        lax.all_gather(expert_down, "fs", axis=1, tiled=True),
        lax.all_gather(shared_gate_cast, "fs", axis=1, tiled=True),
        lax.all_gather(shared_up_cast, "fs", axis=1, tiled=True),
        lax.all_gather(shared_down_cast, "fs", axis=1, tiled=True),
    )
    gate_full, up_full, down_full, sgate_full, sup_full, sdown_full = gathered
    gate_pre = contract(slot_rows, gate_full[0])
    up_pre = contract(slot_rows, up_full[0])
    sgate_part = contract(normed_cols, sgate_full[0])
    sup_part = contract(normed_cols, sup_full[0])
    expert_act = (jax.nn.silu(gate_pre) * up_pre).astype(jnp.bfloat16)
    shared_gate_pre, shared_up_pre = lax.psum((sgate_part, sup_part), "tp")
    shared_act = (jax.nn.silu(shared_gate_pre) * shared_up_pre).astype(jnp.bfloat16)
    expert_out = jnp.dot(expert_act, down_full[0], preferred_element_type=jnp.float32)
    shared_out = jnp.dot(shared_act, sdown_full[0], preferred_element_type=jnp.float32)
    arrived = lax.all_to_all(expert_out, "tp", split_axis=1, concat_axis=0, tiled=True)
    arrived = arrived.reshape(expert_count, capacity, column_width)

    def add_expert(total, inputs):
        source_index, source_rows = inputs
        source_chosen = expert_ids == source_index
        source_weight = jnp.sum(jnp.where(source_chosen, route_weight, 0.0), axis=1)
        source_present = jnp.any(source_chosen, axis=1)
        source_position = jnp.cumsum(source_present.astype(jnp.int32)) - 1
        source_picked = jnp.take(source_rows, jnp.maximum(source_position, 0), axis=0)
        return (
            total + jnp.where(source_present[:, None], source_picked * source_weight[:, None], 0.0),
            None,
        )

    routed_cols, _ = lax.scan(
        add_expert,
        jnp.zeros((token_count, column_width), jnp.float32),
        (jnp.arange(expert_count, dtype=jnp.int32), arrived),
    )
    mixture = (routed_cols + shared_out).astype(jnp.bfloat16)
    return (gate_full, up_full, down_full, sgate_full[0], sup_full[0], sdown_full[0], mixture)

TILE = 16
INNER = 4
VMEM_BYTES = 40000000


def geometry(n, n_fs, experts, rows, columns):
    block = -(-rows // TILE) * TILE
    edge = block - rows
    if n_fs != 2 or experts != n or columns % 128 or not 0 < edge < 8 or block % (TILE * n):
        return None
    if n != INNER * INNER or rows % INNER:
        return None
    return block, edge, block // n


def kernel(
    n,
    block,
    edge,
    piece,
    gate_in,
    up_in,
    down_in,
    sgate_in,
    sup_in,
    sdown_in,
    gain_in,
    tokens_in,
    ids_in,
    scores_in,
    held_pre,
    held_down,
    shared_half,
    mix,
    gain_ref,
    tokens_ref,
    ids_ref,
    scores_ref,
    raw,
    shared_raw,
    rim,
    shared_rim,
    packed_pre,
    packed_down,
    normed,
    gate_acc,
    up_acc,
    act,
    parts,
    plane,
    summed,
    stage,
    relay,
    line,
    small_sem,
    load_sem,
    shared_load_sem,
    rim_sem,
    shared_sem,
    send_sem,
    recv_sem,
    pass_send,
    pass_recv,
    plane_send,
    plane_recv,
    line_send,
    line_recv,
    relay_recv,
):
    routed_in = (gate_in, up_in, down_in)
    shared_in = (sgate_in, sup_in, sdown_in)
    packed = (packed_pre, packed_down)
    held = (held_pre, held_down)
    me = lax.axis_index("tp")
    core = lax.axis_index("fs")
    other = 1 - core
    inner = INNER
    outer = n // inner
    my_a, my_b = me // inner, me % inner
    rows, columns = sgate_in.shape
    chunks = INNER
    chunk = rows // chunks * n
    first = core == 0

    mirror = outer - 1 - my_a
    skip = (my_a + outer // 2) % outer
    beside = my_a + 1 - 2 * (my_a % 2)
    edge_plane = ((my_a + 1) // 2 + 1) % 2
    inner_plane = 1 - edge_plane
    third = edge_plane * mirror + inner_plane * skip
    fourth = edge_plane * skip + inner_plane * mirror

    def mesh_copy(source, target, send, recv, device):
        return pltpu.make_async_remote_copy(
            src_ref=source,
            dst_ref=target,
            send_sem=send,
            recv_sem=recv,
            device_id=device,
            device_id_type=pl.DeviceIdType.MESH,
        )

    def load(m, at):
        here = pl.ds(at * chunk, chunk)
        return pltpu.make_async_copy(routed_in[m].at[here], raw.at[m, here], load_sem.at[m])

    def loaded(m):
        pltpu.make_async_copy(routed_in[m], raw.at[m], load_sem.at[m]).wait()

    def load_shared(m):
        return pltpu.make_async_copy(shared_in[m], shared_raw.at[m], shared_load_sem.at[m])

    def to_peer(k, dst):
        return mesh_copy(
            packed[k].at[dst], held[k].at[me, core], send_sem.at[k], recv_sem.at[k, me], {"tp": dst}
        )

    def from_peer(k, src):
        return mesh_copy(
            packed[k].at[src], held[k].at[src, core], send_sem.at[k], recv_sem.at[k, src], {"tp": src}
        )

    def to_core(k, src, half):
        return mesh_copy(
            held[k].at[src, half],
            held[k].at[src, half],
            pass_send.at[k],
            pass_recv.at[k, src],
            {"fs": other},
        )

    def rim_copy(k):
        here = (pl.ds(0, 2), pl.ds(2, 1))[k]
        return mesh_copy(
            raw.at[here, pl.ds(0, edge * n)], rim.at[here], rim_sem.at[0, k], rim_sem.at[1, k], {"fs": other}
        )

    def shared_rim_copy():
        return mesh_copy(
            shared_raw.at[:, pl.ds(0, 8)], shared_rim, rim_sem.at[0, 2], rim_sem.at[1, 2], {"fs": other}
        )

    def shared_copy(half):
        return mesh_copy(
            shared_half.at[half], shared_half.at[half], shared_sem.at[0], shared_sem.at[1], {"fs": other}
        )

    def to_plane(a, b):
        return mesh_copy(
            parts.at[a, b],
            plane.at[a, my_b],
            plane_send.at[0],
            plane_recv.at[a],
            {"tp": my_a * inner + b},
        )

    def to_beside():
        return mesh_copy(
            stage.at[0], line.at[0], line_send.at[0], line_recv.at[0], {"tp": beside * inner + my_b}
        )

    def to_relay(k):
        return mesh_copy(
            stage.at[k + 1],
            relay.at[k],
            line_send.at[0],
            relay_recv.at[k],
            {"tp": beside * inner + my_b},
        )

    def to_line(k, a):
        return mesh_copy(
            stage.at[k + 1], line.at[1], line_send.at[0], line_recv.at[1], {"tp": a * inner + my_b}
        )

    def assemble(value, tail):
        cut = block - TILE
        body = jnp.where(first, value[0:cut], value[edge : cut + edge])
        rest = jnp.where(
            first,
            jnp.concatenate([value[cut:rows], tail[0:edge]], axis=0),
            jnp.concatenate(
                [value[cut + edge : rows], jnp.zeros((2 * edge, columns), jnp.float32)], axis=0
            ),
        )
        return cut, body, rest

    smalls = [
        pltpu.make_async_copy(source, target, small_sem.at[at])
        for at, (source, target) in enumerate(
            (
                (gain_in, gain_ref),
                (tokens_in, tokens_ref),
                (ids_in, ids_ref),
                (scores_in, scores_ref),
            )
        )
    ]
    smalls[0].start()
    for m in range(3):
        load_shared(m).start()
    for m in range(3):
        for at in range(chunks):
            load(m, at).start()
    for copy in smalls[1:]:
        copy.start()

    barrier = pltpu.get_barrier_semaphore()
    pl.semaphore_signal(
        barrier, inc=1, device_id={"fs": other}, device_id_type=pl.DeviceIdType.MESH
    )

    def greet(step, carry):
        pl.semaphore_signal(
            barrier,
            inc=1,
            device_id={"tp": (me + step) % n},
            device_id_type=pl.DeviceIdType.MESH,
        )
        return carry

    lax.fori_loop(1, n, greet, 0)
    smalls[0].wait()
    for m in range(3):
        load_shared(m).wait()
    loaded(0)
    loaded(1)
    pl.semaphore_wait(barrier, n)

    @pl.when(core == 1)
    def _():
        shared_rim_copy().start()
        rim_copy(0).start()

    @pl.when(core == 0)
    def _():
        shared_rim_copy().wait_recv()
        rim_copy(0).wait_recv()

    gain = gain_ref[...]
    for m in range(3):
        scale = gain if m < 2 else jnp.ones_like(gain)
        cut, body, rest = assemble(shared_raw[m], shared_rim[m])
        shared_half[core, m, 0:cut] = (body * scale).astype(jnp.bfloat16)
        shared_half[core, m, cut:block] = (rest * scale).astype(jnp.bfloat16)

    def pack(m, dst, target):
        scale = gain if m < 2 else jnp.ones_like(gain)
        cut = block - TILE
        start = dst + core * (edge * n)
        body = raw[m, pl.ds(start, cut, stride=n), :]
        end = raw[m, pl.ds(dst + cut * n, rows - cut, stride=n), :]
        head = rim[m, pl.ds(dst, edge, stride=n), :]
        rest = jnp.where(
            first,
            jnp.concatenate([end, head], axis=0),
            jnp.concatenate([end[edge:], jnp.zeros((2 * edge, columns), jnp.float32)], axis=0),
        )
        target[0:cut] = (body * scale).astype(jnp.bfloat16)
        target[cut:block] = (rest * scale).astype(jnp.bfloat16)
        target[block : block + piece] = shared_half[
            core, m, pl.ds(pl.multiple_of(dst * piece, TILE), piece)
        ]

    def pack_all(k, dst):
        if k == 0:
            for m in range(2):
                pack(m, dst, packed_pre.at[dst, m])
        else:
            pack(2, dst, packed_down.at[dst])

    def member(plane_at, shift):
        column = (my_b + shift) % 2 + 2 * ((my_b // 2 + shift // 2) % 2)
        return plane_at * inner + column

    def shift_of(k, step, rising):
        if k == 0:
            turn = step + rising * (inner - 1 - 2 * step)
            return (2 * turn + 1 - turn // 2) % inner
        return (1 + 2 * step + step // 2) % inner

    def peer_to(k, plane_at, step):
        return member(plane_at, shift_of(k, step, (plane_at > my_a).astype(jnp.int32)))

    def peer_from(k, plane_at, step):
        return member(plane_at, shift_of(k, step, (plane_at < my_a).astype(jnp.int32)))

    def peer_own(step):
        return member(my_a, step + 1)

    def send_plane(k, plane_at, start):
        def send(step, carry):
            dst = peer_to(k, plane_at, step)
            pack_all(k, dst)
            if start:
                to_peer(k, dst).start()
            return carry

        lax.fori_loop(0, inner, send, 0)

    def send_own(k):
        def send(step, carry):
            dst = peer_own(step)
            pack_all(k, dst)
            to_peer(k, dst).start()
            return carry

        lax.fori_loop(0, inner - 1, send, 0)

    def launch(k, plane_at):
        def send(step, carry):
            to_peer(k, peer_to(k, plane_at, step)).start()
            return carry

        lax.fori_loop(0, inner, send, 0)

    for plane_at in (mirror, skip, beside):
        send_plane(0, plane_at, True)
    send_own(0)
    loaded(2)

    @pl.when(core == 1)
    def _():
        rim_copy(1).start()

    @pl.when(core == 0)
    def _():
        rim_copy(1).wait_recv()

    send_plane(1, beside, True)
    send_own(1)
    for plane_at in (skip, mirror):
        send_plane(1, plane_at, False)

    @pl.when(inner_plane == 1)
    def _():
        launch(1, skip)
        launch(1, mirror)

    for m in range(2):
        pack(m, me, held_pre.at[me, core, m])
    pack(2, me, held_down.at[me, core])
    shared_copy(core).start()

    for copy in smalls[1:]:
        copy.wait()
    tokens = tokens_ref[...].astype(jnp.float32)
    mean = jnp.mean(tokens * tokens, axis=1, keepdims=True)
    scaled = (tokens * lax.rsqrt(mean + EPSILON)).astype(jnp.bfloat16)
    for i in range(n):
        normed[i] = scaled[:, i * columns : (i + 1) * columns]
    scores = scores_ref[...]
    weights = ROUTED_SCALE * scores / jnp.sum(scores, axis=0, keepdims=True)
    weight = jnp.sum(jnp.where(ids_ref[...] == me, weights, 0.0), axis=0, keepdims=True)
    weight = jnp.transpose(jnp.broadcast_to(weight, (8, weight.shape[1])))[:, 0:1]
    gate_acc[...] = jnp.zeros_like(gate_acc)
    up_acc[...] = jnp.zeros_like(up_acc)

    hidden = 2 * (block + piece)

    def arrive(k, src, local):
        if not local:
            from_peer(k, src).wait_recv()
        to_core(k, src, core).start()

    def add(src):
        to_core(0, src, other).wait_recv()
        for m, acc in ((0, gate_acc), (1, up_acc)):
            acc[...] += lax.dot_general(
                normed[src],
                held_pre[src, :, m].reshape(hidden, columns),
                (((1,), (1,)), ((), ())),
                preferred_element_type=jnp.float32,
            )

    def part(src):
        to_core(1, src, other).wait_recv()
        a, b = src // inner, src % inner
        parts[a, b] = jnp.dot(
            act[...], held_down[src].reshape(hidden, columns), preferred_element_type=jnp.float32
        ).astype(jnp.bfloat16)

        @pl.when(b != my_b)
        def _():
            to_plane(a, b).start()

    def stream(k, use, planes, after):
        arrive(k, me, True)
        before = me
        for at, plane_at in enumerate(planes):

            def one(step, waiting):
                src = peer_own(step) if at == 0 else peer_from(k, plane_at, step)
                arrive(k, src, False)
                use(waiting)
                return src

            before = lax.fori_loop(0, inner - 1 if at == 0 else inner, one, before)
            after(at)
        use(before)

    stream(0, add, (my_a, third, beside, fourth), lambda at: None)

    @pl.when(edge_plane == 1)
    def _():
        launch(1, mirror)
        launch(1, skip)

    gate_pre = gate_acc[...]
    place = lax.broadcasted_iota(jnp.int32, gate_pre.shape, 1) % (block + piece)
    share = jnp.where(place < block, weight, 1.0)
    act[...] = (gate_pre / (1.0 + jnp.exp(-gate_pre)) * up_acc[...] * share).astype(jnp.bfloat16)

    def plane_sum(a):
        mesh_copy(
            parts.at[a, pl.ds(0, inner - 1)],
            plane.at[a, pl.ds(0, inner - 1)],
            plane_send.at[0],
            plane_recv.at[a],
            {"fs": other},
        ).wait_recv()
        result = parts[a, my_b].astype(jnp.float32)
        for db in range(1, inner):
            result = result + plane[a, (my_b + db) % inner].astype(jnp.float32)
        return result

    def flush_beside():
        stage[0] = plane_sum(beside).astype(jnp.bfloat16)
        to_beside().start()

    def flush(k, a):
        summed[...] = plane_sum(a)

        @pl.when(edge_plane == 1)
        def _():
            stage[k + 1] = summed[...].astype(jnp.bfloat16)
            to_relay(k).start()

        @pl.when(inner_plane == 1)
        def _():
            to_relay(k).wait_recv()
            stage[k + 1] = (summed[...] + relay[k].astype(jnp.float32)).astype(jnp.bfloat16)
            to_line(k, a).start()

    stream(1, part, (my_a, beside, third), lambda at: None)

    def last(step, carry):
        src = peer_from(1, fourth, step)
        arrive(1, src, False)
        part(src)
        return carry

    lax.fori_loop(0, inner - 2, last, 0)
    flush_beside()
    lax.fori_loop(inner - 2, inner - 1, last, 0)
    flush(0, third)
    lax.fori_loop(inner - 1, inner, last, 0)
    flush(1, fourth)
    summed[...] = plane_sum(my_a)
    to_beside().wait_recv()
    summed[...] += line[0].astype(jnp.float32)
    shared_copy(other).wait_recv()
    to_line(0, my_a).wait_recv()
    mix[...] = (summed[...] + line[1].astype(jnp.float32)).astype(jnp.bfloat16)

    for k in range(2):
        mesh_copy(
            packed[k].at[pl.ds(0, n - 1)],
            packed[k].at[pl.ds(0, n - 1)],
            send_sem.at[k],
            recv_sem.at[k, 0],
            {"fs": other},
        ).wait_send()
        mesh_copy(
            held[k].at[:, core], held[k].at[:, core], pass_send.at[k], pass_recv.at[k, 0], {"fs": other}
        ).wait_send()

    @pl.when(core == 1)
    def _():
        shared_rim_copy().wait_send()
        rim_copy(0).wait_send()
        rim_copy(1).wait_send()

    shared_copy(core).wait_send()
    mesh_copy(
        parts.at[:, pl.ds(0, inner - 1)],
        plane.at[:, pl.ds(0, inner - 1)],
        plane_send.at[0],
        plane_recv.at[0],
        {"fs": other},
    ).wait_send()
    mesh_copy(stage, stage, line_send.at[0], line_recv.at[0], {"fs": other}).wait_send()


def store(
    n, block, held_pre, held_down, shared_half, mix, gate_out, up_out, down_out, sgate_out, sup_out, sdown_out, mix_out, sem
):
    columns = mix.shape[1]
    sizes = (block, gate_out.shape[0] - block)
    routed_out = (gate_out, up_out, down_out)
    shared_out = (sgate_out, sup_out, sdown_out)
    for m in range(3):
        for src in range(n):
            for half in range(2):
                source = held_down.at[src, half] if m == 2 else held_pre.at[src, half, m]
                pltpu.make_async_copy(
                    source.at[pl.ds(0, sizes[half])],
                    routed_out[m].at[pl.ds(half * block, sizes[half]), pl.ds(src * columns, columns)],
                    sem.at[m],
                ).start()
        for half in range(2):
            pltpu.make_async_copy(
                shared_half.at[half, m, pl.ds(0, sizes[half])],
                shared_out[m].at[pl.ds(half * block, sizes[half])],
                sem.at[3 + m],
            ).start()
    pltpu.make_async_copy(mix, mix_out, sem.at[6]).start()
    for at, target in enumerate((*routed_out, *shared_out, mix_out)):
        pltpu.make_async_copy(target, target, sem.at[at]).wait()


def on_device(n, shape, gate, up, down, sgate, sup, sdown, gain, tokens, ids, scores):
    block, edge, piece = shape
    experts, rows, columns = gate.shape
    count, width = tokens.shape
    unit = block + piece
    hidden = 2 * unit
    inner, outer = INNER, n // INNER
    sem = pltpu.SemaphoreType.DMA
    hbm = pl.BlockSpec(memory_space=pltpu.HBM)
    vmem = pl.BlockSpec(memory_space=pltpu.VMEM)
    bf16, f32 = jnp.bfloat16, jnp.float32
    results = pl.pallas_call(
        functools.partial(kernel, n, block, edge, piece),
        out_shape=(
            pltpu.VMEM((n, 2, 2, unit, columns), bf16),
            pltpu.VMEM((n, 2, unit, columns), bf16),
            pltpu.VMEM((2, 3, block, columns), bf16),
            pltpu.VMEM((count, columns), bf16),
        ),
        in_specs=[hbm] * 10,
        out_specs=(vmem,) * 4,
        scratch_shapes=[
            pltpu.VMEM((1, columns), f32),
            pltpu.VMEM(tokens.shape, bf16),
            pltpu.VMEM(ids.shape[::-1], jnp.int32),
            pltpu.VMEM(scores.shape[::-1], f32),
            pltpu.VMEM((3, n * rows, columns), f32),
            pltpu.VMEM((3, rows, columns), f32),
            pltpu.VMEM((3, n * edge, columns), f32),
            pltpu.VMEM((3, 8, columns), f32),
            pltpu.VMEM((n, 2, unit, columns), bf16),
            pltpu.VMEM((n, unit, columns), bf16),
            pltpu.VMEM((n, count, columns), bf16),
            pltpu.VMEM((count, hidden), f32),
            pltpu.VMEM((count, hidden), f32),
            pltpu.VMEM((count, hidden), bf16),
            pltpu.VMEM((outer, inner, count, columns), bf16),
            pltpu.VMEM((outer, inner, count, columns), bf16),
            pltpu.VMEM((count, columns), f32),
            pltpu.VMEM((3, count, columns), bf16),
            pltpu.VMEM((2, count, columns), bf16),
            pltpu.VMEM((2, count, columns), bf16),
            sem((4,)),
            sem((3,)),
            sem((3,)),
            sem((2, 3)),
            sem((2,)),
            sem((2,)),
            sem((2, n)),
            sem((2,)),
            sem((2, n)),
            sem((1,)),
            sem((outer,)),
            sem((1,)),
            sem((2,)),
            sem((2,)),
        ],
        compiler_params=pltpu.CompilerParams(
            collective_id=0, has_side_effects=True, vmem_limit_bytes=VMEM_BYTES
        ),
    )(
        *[
            pltpu.with_memory_space_constraint(array, pltpu.HBM)
            for array in (
                *[
                    jnp.transpose(array, (1, 0, 2)).reshape(rows * n, columns)
                    for array in (gate, up, down)
                ],
                sgate,
                sup,
                sdown,
                gain[None, :],
                tokens,
                ids.T,
                scores.T,
            )
        ]
    )
    full = jax.ShapeDtypeStruct((2 * rows, width), bf16)
    thin = jax.ShapeDtypeStruct((2 * rows, columns), bf16)
    whole = pl.pallas_call(
        functools.partial(store, n, block),
        out_shape=(full, full, full, thin, thin, thin, jax.ShapeDtypeStruct((count, columns), bf16)),
        in_specs=[vmem] * 4,
        out_specs=(hbm,) * 7,
        scratch_shapes=[sem((7,))],
        compiler_params=pltpu.CompilerParams(vmem_limit_bytes=VMEM_BYTES),
    )(*[pltpu.with_memory_space_constraint(array, pltpu.VMEM) for array in results])
    return (*[array[None] for array in whole[:3]], *whole[3:])


def body(n, n_fs, *args):
    experts, rows, columns = args[0].shape
    shape = geometry(n, n_fs, experts, rows, columns)
    if shape is None:
        return plain_on_device(*args)
    return on_device(n, shape, *args)


def solution(mesh):
    placed = (
        P(None, "fs", "tp"),
        P(None, "fs", "tp"),
        P(None, "fs", "tp"),
        P("fs", "tp"),
        P("fs", "tp"),
        P("fs", "tp"),
        P("tp"),
        P("fs", None),
        P("fs", None),
        P("fs", None),
    )
    return jax.shard_map(
        functools.partial(body, mesh.shape["tp"], mesh.shape["fs"]),
        mesh=mesh,
        in_specs=placed,
        out_specs=(
            P("tp", None, None),
            P("tp", None, None),
            P("tp", None, None),
            P(None, "tp"),
            P(None, "tp"),
            P(None, "tp"),
            P("fs", "tp"),
        ),
        check_vma=False,
    )
```
